128 devices in a mesh: sp: 16 (over z, y), dp: 8 (over x, core).
Axes of the slice: x: 4, y: 4, z: 4, core: 2. Of those that a mesh axis runs over, the one named last changes fastest.
Arguments:
- queries: bfloat16 [8, 2048, 16, 128], P('dp', 'sp'), may hold values from -7 to 7
- key_vectors: bfloat16 [8, 2048, 16, 128], P('dp', 'sp'), may hold values from -6 to 6
- value_vectors: bfloat16 [8, 2048, 16, 128], P('dp', 'sp'), may hold values from -6 to 6
- head_lambda: float32 [16], P('sp'), may hold values from 0.3 to 0.8
- head_gain: float32 [128], replicated, may hold values from 0.1 to 1.9
- residual: bfloat16 [8, 2048, 2048], P('dp', 'sp'), may hold values from -6 to 6
- out_weight: bfloat16 [2048, 2048], replicated, may hold values from -0.125 to 0.125
- mix_gain: float32 [2048], replicated, may hold values from 0.1 to 1.9
- pre_gain: float32 [2048], replicated, may hold values from 0.1 to 1.9
- post_gain: float32 [2048], replicated, may hold values from 0.1 to 1.9
- routes: int32 [8, 2048, 4], P('dp', 'sp'), may hold values from 0 to 127, all different within a row; in each aligned block of 128 rows (0 to 127, 128 to 255, ..., all dimensions but the last counted through in order) at most 6 rows name the same one
- route_weights: float32 [8, 2048, 4], P('dp', 'sp'), may hold values from 0.25 to 1
- expert_gate: bfloat16 [128, 2048, 512], P(('sp', 'dp')), may hold values from -0.125 to 0.125
- expert_up: bfloat16 [128, 2048, 512], P(('sp', 'dp')), may hold values from -0.125 to 0.125
- expert_down: bfloat16 [128, 512, 2048], P(('sp', 'dp')), may hold values from -0.25 to 0.25
- shared_gate: bfloat16 [2048, 512], replicated, may hold values from -0.125 to 0.125
- shared_up: bfloat16 [2048, 512], replicated, may hold values from -0.125 to 0.125
- shared_down: bfloat16 [512, 2048], replicated, may hold values from -0.25 to 0.25
Outputs:
- output: bfloat16 [8, 2048, 2048], P('dp', 'sp')
The draws below stay inside these ranges and needn't reach their ends.
Inputs may be any that keep to these rules, and one draw needn't show every extreme that they name: `routes`: among the tokens of one device (aligned blocks of 128 positions), no expert is named more than 6 times; in some block some expert is named exactly 6 times. Each token names 4 different experts.
All inputs are finite; a program needn't handle non-finite values.
Results may differ from the reference program's by a relative error of at most 0.0075.
Values may be sent and summed in bfloat16 or wider, within the bound.
A program may use at most 128 MiB of HBM per device.

```python
import math
import jax
import jax.numpy as jnp
import numpy as np
from jax import lax

D = 2048
HEADS = 16
HD = 64
VD = 128
FF = 512
TOP_K = 4
TOK_DEV = 128
LEN = 2048
SEQS = 8
EXPERTS = 128
CAP = 6


def draw_queries(key, part):
    shape = (SEQS, LEN, HEADS, 2 * HD)
    base_key = jax.random.fold_in(key, 11)
    drawn = jnp.clip(1.75 * jax.random.normal(base_key, shape, jnp.float32), -7.0, 7.0)
    return drawn.astype(jnp.bfloat16)


def draw_key_vectors(key, part):
    shape = (SEQS, LEN, HEADS, 2 * HD)
    base_key = jax.random.fold_in(key, 13)
    drawn = jnp.clip(jax.random.normal(base_key, shape, jnp.float32), -6.0, 6.0)
    return drawn.astype(jnp.bfloat16)


def levels(key, dims, cuts, least, top_value):
    def one(position, parts):
        draws = jax.random.uniform(jax.random.fold_in(jax.random.fold_in(key, 6), position), (parts,), jnp.float32, least / len(cuts), top_value / len(cuts))
        return jnp.repeat(jnp.exp(draws), dims[position] // parts).reshape((-1,) + (1,) * (len(dims) - position - 1))

    level = one(*cuts[0])
    for cut in cuts[1:]:
        level = level * one(*cut)
    return level


def deal_out(rng, own, number, rows, amount, top, reach, slope):
    sequence = jax.random.permutation(rng, amount)
    heavy_load, common = portions_of(amount, rows * top, reach, slope, True), portions_of(amount, rows * top, reach, slope, False)
    places = jnp.arange(amount)

    def named(lengths, rotation):
        used = int((lengths > 0).sum())
        fixed = max(1, used // 4)
        passed = fixed + (places - fixed + rotation * (used - fixed)) % max(1, amount - fixed)
        return jnp.zeros((amount,), jnp.int32).at[sequence[jnp.where(places < fixed, places, passed)]].set(jnp.asarray(lengths, jnp.int32))

    lengths = jnp.where(number % 4 == 0, named(heavy_load, number // 4), named(common, number - number // 4 - 1))
    mixed = jax.random.permutation(jax.random.fold_in(own, 3), amount)
    source_of, sink = mixed[0:amount // 2 * 2:2], mixed[1:amount // 2 * 2:2]
    room = jnp.minimum(lengths[source_of] - 1, reach - lengths[sink]) // 2
    room = jnp.where((source_of == sequence[0]) | (sink == sequence[0]) | (lengths[sink] == 0), 0, jnp.maximum(room, 0))
    passed = jax.random.randint(jax.random.fold_in(own, 4), (amount // 2,), 0, 1 << 20) % (room + 1)
    lengths = lengths.at[source_of].add(-passed).at[sink].add(passed)
    members = jnp.searchsorted(jnp.cumsum(lengths), jnp.arange(rows * top), side="right").astype(jnp.int32)
    listing = members.reshape(top, rows).T
    listing = listing[jax.random.permutation(jax.random.fold_in(own, 1), rows)]
    rotation = jax.random.randint(jax.random.fold_in(own, 2), (rows, 1), 0, top)
    return jnp.take_along_axis(listing, (jnp.arange(top)[None, :] + rotation) % top, axis=1)


def portions_of(count, total, reach, lean, full):
    weights = [(1 << 20) // math.isqrt(grade ** lean) + 1 for grade in range(1, count + 1)]
    largest = reach if full else min(reach, max(-(-total // count), total * weights[0] // sum(weights)))
    least = 1 if total - largest >= count - 1 else 0
    counts, spare = [largest] + [least] * (count - 1), total - largest - least * (count - 1)
    while spare > 0:
        candidates = [i for i in range(1, count) if counts[i] < largest] or [i for i in range(1, count) if counts[i] < reach]
        whole, remaining = sum([weights[i] for i in candidates]), spare
        for i in candidates:
            extra = min(reach - counts[i], max(1, remaining * weights[i] // whole), spare)
            counts[i] = counts[i] + extra
            spare = spare - extra
    return np.array(counts)


def bell_draw(rng, dims, spread, reach, pieces=(), held_as=jnp.bfloat16):
    values = spread * jax.random.normal(rng, dims, jnp.float32)
    if pieces:
        values = values * levels(rng, dims, pieces, -0.22, 0.18)
    return jnp.clip(values, -reach, reach).astype(held_as)


def setup_inputs(seed: int = 0) -> dict:
    key_list = jax.random.split(jax.random.key(seed), 19)
    queries = draw_queries(jax.random.fold_in(key_list[18], 71), 0)
    key_vectors = draw_key_vectors(jax.random.fold_in(key_list[18], 71), 0)
    value_vectors = bell_draw(key_list[2], (SEQS, LEN, HEADS, VD), 1.0, 6.0, ((0, 8), (1, 16)))
    head_lambda = jnp.clip(0.3 + 0.5 * jax.random.uniform(key_list[3], (HEADS,), jnp.float32) ** levels(key_list[3], (HEADS,), ((0, 16),), -0.2, 0.2), 0.3, 0.8)
    head_gain = jnp.clip(1.0 + 0.18 * jax.random.normal(key_list[4], (VD,), jnp.float32), 0.1, 1.9)
    residual = bell_draw(key_list[5], (SEQS, LEN, D), 1.0, 6.0, ((0, 8), (1, 16)))
    out_weight = bell_draw(key_list[6], (HEADS * VD, D), (HEADS * VD) ** -0.5, 0.125)
    mix_gain = jnp.clip(1.0 + 0.18 * jax.random.normal(key_list[7], (D,), jnp.float32), 0.1, 1.9)
    pre_gain = jnp.clip(1.0 + 0.18 * jax.random.normal(key_list[8], (D,), jnp.float32), 0.1, 1.9)
    post_gain = jnp.clip(1.0 + 0.18 * jax.random.normal(key_list[9], (D,), jnp.float32), 0.1, 1.9)
    routes_keys = jax.random.split(jax.random.fold_in(key_list[10], 1), SEQS * LEN // TOK_DEV)
    routes_turns = jax.random.permutation(jax.random.fold_in(key_list[10], 3), SEQS * LEN // TOK_DEV)
    routes = jax.vmap(lambda own, number: deal_out(jax.random.fold_in(key_list[10], 2), own, number, TOK_DEV, EXPERTS, TOP_K, CAP, 2))(routes_keys, routes_turns).reshape((SEQS, LEN, TOP_K))
    route_weights = jnp.clip(0.25 + 0.75 * jax.random.uniform(key_list[11], (SEQS, LEN, TOP_K), jnp.float32) ** levels(key_list[11], (SEQS, LEN, TOP_K), ((0, 8), (1, 16)), -0.2, 0.2), 0.25, 1.0)
    expert_gate = bell_draw(key_list[12], (EXPERTS, D, FF), D ** -0.5, 0.125, ((0, 128),))
    expert_up = bell_draw(key_list[13], (EXPERTS, D, FF), D ** -0.5, 0.125, ((0, 128),))
    expert_down = bell_draw(key_list[14], (EXPERTS, FF, D), FF ** -0.5, 0.25, ((0, 128),))
    shared_gate = bell_draw(key_list[15], (D, FF), D ** -0.5, 0.125)
    shared_up = bell_draw(key_list[16], (D, FF), D ** -0.5, 0.125)
    shared_down = bell_draw(key_list[17], (FF, D), FF ** -0.5, 0.25)
    return dict(queries=queries, key_vectors=key_vectors, value_vectors=value_vectors, head_lambda=head_lambda, head_gain=head_gain, residual=residual, out_weight=out_weight, mix_gain=mix_gain, pre_gain=pre_gain, post_gain=post_gain, routes=routes, route_weights=route_weights, expert_gate=expert_gate, expert_up=expert_up, expert_down=expert_down, shared_gate=shared_gate, shared_up=shared_up, shared_down=shared_down)


epsilon = 1e-06

def rms_scale(values_in, gain):
    return values_in * lax.rsqrt(lax.optimization_barrier(jnp.mean(values_in * values_in, axis=-1, keepdims=True)) + epsilon) * gain

def feed_forward(rows, gate_w, up_w, down_w):
    gate_val = jnp.dot(rows, gate_w, preferred_element_type=jnp.float32)
    up_val = jnp.dot(rows, up_w, preferred_element_type=jnp.float32)
    hidden = (jax.nn.silu(gate_val) * up_val).astype(jnp.bfloat16)
    return jnp.dot(hidden, down_w, preferred_element_type=jnp.float32).astype(jnp.bfloat16)

def attend_sequence(query_seq, key_seq, value_seq, head_lambda, head_gain):
    length = query_seq.shape[0]
    head_count = query_seq.shape[1]
    head_size = query_seq.shape[2] // 2
    block_rows = min(512, length)
    block_count = length // block_rows
    query_blocks = query_seq.astype(jnp.float32).reshape(block_count, block_rows, head_count, 2, head_size)
    key_all = key_seq.astype(jnp.float32).reshape(length, head_count, 2, head_size)
    value_all = value_seq.astype(jnp.float32)
    key_pos = jnp.arange(length, dtype=jnp.int32)

    def one_block(inputs):
        query_block, block_index = inputs
        scores = jnp.einsum('qhmd,khmd->hmqk', query_block, key_all) * head_size ** (-0.5)
        query_pos = block_index * block_rows + jnp.arange(block_rows, dtype=jnp.int32)
        causal = key_pos[None, :] <= query_pos[:, None]
        scores = jnp.where(causal, scores, -jnp.inf)
        maxima = lax.optimization_barrier(jnp.max(scores, axis=-1, keepdims=True))
        exponent = jnp.exp(scores - maxima)
        softmax_both = exponent / lax.optimization_barrier(jnp.sum(exponent, axis=-1, keepdims=True))
        mixture = softmax_both[:, 0] - head_lambda[:, None, None] * softmax_both[:, 1]
        mixture_low = lax.optimization_barrier(mixture.astype(jnp.bfloat16)).astype(jnp.float32)
        head_output = jnp.einsum('hqk,khe->qhe', mixture_low, value_all)
        return rms_scale(head_output, head_gain).astype(jnp.bfloat16)
    outputs = lax.map(one_block, (query_blocks, jnp.arange(block_count, dtype=jnp.int32)))
    return outputs.reshape(length, head_count, -1)

def reference(queries, key_vectors, value_vectors, head_lambda, head_gain, residual, out_weight, mix_gain, pre_gain, post_gain, routes, route_weights, expert_gate, expert_up, expert_down, shared_gate, shared_up, shared_down):
    heads_out = lax.map(lambda inputs: attend_sequence(inputs[0], inputs[1], inputs[2], head_lambda, head_gain), (queries, key_vectors, value_vectors))
    token_total = SEQS * LEN
    flat_heads = heads_out.reshape(token_total, HEADS * VD)
    mixed_rows = jnp.dot(flat_heads, out_weight, preferred_element_type=jnp.float32)
    updated = (residual.reshape(token_total, D).astype(jnp.float32) + rms_scale(mixed_rows, mix_gain)).astype(jnp.bfloat16)
    normed = rms_scale(updated.astype(jnp.float32), pre_gain).astype(jnp.bfloat16)
    shared_out = feed_forward(normed, shared_gate, shared_up, shared_down)
    block_total = token_total // TOK_DEV
    assign_block = TOK_DEV * TOP_K
    flat_routes = routes.reshape(block_total, assign_block).astype(jnp.int32)
    one_hot = (flat_routes[:, :, None] == jnp.arange(EXPERTS, dtype=jnp.int32)[None, None, :]).astype(jnp.int32)
    earlier = jnp.cumsum(one_hot, axis=1) - one_hot
    rank_index = lax.optimization_barrier(jnp.sum(earlier * one_hot, axis=2))
    block_ids = jnp.arange(block_total, dtype=jnp.int32)[:, None]
    slot_index = (flat_routes * (block_total * CAP) + block_ids * CAP + rank_index).reshape(-1)
    assign_ids = jnp.arange(block_total * assign_block, dtype=jnp.int32)
    source_table = jnp.zeros((EXPERTS * block_total * CAP,), jnp.int32).at[slot_index].set(assign_ids)
    rows_per_expert = source_table.reshape(EXPERTS, block_total * CAP) // TOP_K

    def run_expert(inputs):
        row_ids, gate_w, up_w, down_w = inputs
        return feed_forward(normed[row_ids], gate_w, up_w, down_w)
    expert_out = lax.map(run_expert, (rows_per_expert, expert_gate, expert_up, expert_down))
    picked = expert_out.reshape(EXPERTS * block_total * CAP, D)[slot_index]
    routed = lax.optimization_barrier(jnp.sum(picked.astype(jnp.float32).reshape(token_total, TOP_K, D) * route_weights.reshape(token_total, TOP_K, 1), axis=1))
    combined = routed + shared_out.astype(jnp.float32)
    output = (updated.astype(jnp.float32) + rms_scale(combined, post_gain)).astype(jnp.bfloat16)
    return output.reshape(SEQS, LEN, D)
```

```python
import functools

import jax
import jax.numpy as jnp
import numpy as np
from jax import lax
from jax.experimental import pallas as pl
from jax.experimental.pallas import tpu as pltpu
from jax.sharding import PartitionSpec as P

MESH = pl.DeviceIdType.MESH
EPS = 1e-06
F32, BF16, I32 = jnp.float32, jnp.bfloat16, jnp.int32


def digits(k):
    return k // 32, (k // 8) % 4, (k // 2) % 4, k % 2


def link_load(k):
    load = np.zeros(6)
    dz, dy, dx, _ = digits(k)
    for i, d in enumerate((dx, dy, dz)):
        if d in (1, 2):
            load[2 * i] += 1
        if d in (2, 3):
            load[2 * i + 1] += 1
    return load


def first_link(k):
    dz, dy, dx, _ = digits(k)
    for i, d in enumerate((dx, dy, dz)):
        if d:
            return i, d
    return 3, 0


def balanced_order(offsets):
    left, total, out, last = list(offsets), np.zeros(6), [], None
    while left:

        def cost(k):
            t = total + link_load(k)
            return t.max() - t.min() + (0.5 if last is not None and first_link(k) == last else 0)

        k = min(left, key=cost)
        left.remove(k)
        out.append(k)
        total = total + link_load(k)
        last = first_link(k)
    return out


SP_ORDER = [k // 8 for k in balanced_order([8 * s for s in range(1, 16)])]
ALL_ORDER = [0] + balanced_order(range(1, 128))


def shifted(sp, dp, k, sign):
    dz, dy, dx, dc = digits(k)
    if sign < 0:
        dz, dy, dx, dc = -dz % 4, -dy % 4, -dx % 4, -dc % 2
    rem = lax.rem
    nsp = rem(sp // 4 + dz, 4) * 4 + rem(rem(sp, 4) + dy, 4)
    ndp = rem(dp // 2 + dx, 4) * 2 + rem(rem(dp, 2) + dc, 2)
    return nsp, ndp


def landed(ref, sem):
    pltpu.make_async_copy(ref, ref, sem).wait()


def dot(a, b):
    return jnp.dot(a, b, preferred_element_type=F32)


def rms(v, gain):
    return v * lax.rsqrt(jnp.mean(v * v, axis=-1, keepdims=True) + EPS) * gain


def layer_kernel(
    q_ref, k_ref, v_ref, lam_ref, hgain_ref, res_ref, mixg_ref, preg_ref, postg_ref,
    routes_ref, rw_ref, order_ref, perm_ref, permt_ref,
    wo_hbm, eg_hbm, eu_hbm, ed_hbm, sg_hbm, su_hbm, sd_hbm,
    out_ref,
    wo, eg, eu, ed, sg, su, sd,
    spread, qkv_send, qkv_recv, vext, head_send, head_recv, acc,
    x4, pick, slab_send, slab_recv, res_send, res_recv, whi, wlo, xs, upd, shared, r0s,
    wsem, qs_sem, qr_sem, hs_sem, hr_sem, ds_sem, dr_sem, rs_sem, rr_sem,
):
    sp, dp = lax.axis_index("sp"), lax.axis_index("dp")
    loads = [
        pltpu.make_async_copy(src, dst, wsem.at[i])
        for i, (src, dst) in enumerate(
            ((wo_hbm, wo), (sg_hbm, sg), (su_hbm, su), (sd_hbm, sd), (eg_hbm, eg), (eu_hbm, eu), (ed_hbm, ed))
        )
    ]
    barrier = pltpu.get_barrier_semaphore()

    @pl.loop(1, 128)
    def _(k):
        peer = lax.rem(sp * 8 + dp + k, 128)
        pl.semaphore_signal(barrier, inc=1, device_id=(peer // 8, lax.rem(peer, 8)), device_id_type=MESH)

    for part, ref in enumerate((q_ref, k_ref, v_ref)):
        spread[part] = ref[...].reshape(2048, 128).astype(F32)
    for h in range(16):
        for part in range(3):
            qkv_send[h, part] = spread[part, pl.ds(h, 128, stride=16), :].astype(BF16)
    pl.semaphore_wait(barrier, 127)
    for i, d in enumerate(SP_ORDER):
        to, _ = shifted(sp, dp, 8 * d, 1)
        pltpu.make_async_remote_copy(
            qkv_send.at[to], qkv_recv.at[sp], qs_sem.at[i], qr_sem.at[i],
            device_id=(to, dp), device_id_type=MESH,
        ).start()
    for load in loads:
        load.start()
    qkv_recv[sp] = qkv_send[sp]

    oz, oy, ox, oc = (order_ref[i : i + 1, :] for i in range(4))
    mz, my, mx, mc = sp // 4, lax.rem(sp, 4), dp // 2, lax.rem(dp, 2)
    expert = ((oz + mz) & 3) * 32 + ((oy + my) & 3) * 8 + ((ox + mx) & 3) * 2 + ((oc + mc) & 1)
    row_i = lax.broadcasted_iota(I32, (128, 128), 0)
    col_i = lax.broadcasted_iota(I32, (128, 128), 1)
    hots = [routes_ref[:, j : j + 1] == expert for j in range(4)]
    members = sum(h.astype(F32) for h in hots).astype(BF16)
    earlier = dot((col_i < row_i).astype(F32).astype(BF16), members)
    place = earlier + 24.0 * col_i.astype(F32)
    eye = col_i == row_i
    rows_j = []
    for j in range(4):
        r0 = jnp.sum(jnp.where(hots[j], place, 0.0), axis=1, keepdims=True)
        r0s[:, j : j + 1] = r0.astype(I32)
        r0_row = jnp.sum(jnp.where(eye, r0, 0.0), axis=0, keepdims=True).astype(I32)
        rows_j.append(jnp.concatenate([r0_row + 6 * q for q in range(4)], axis=1))

    @pl.loop(0, 24)
    def _(c):
        base = pl.multiple_of(c * 128, 128)
        row = lax.broadcasted_iota(I32, (128, 512), 0) + base
        hit = (row == rows_j[0]) | (row == rows_j[1]) | (row == rows_j[2]) | (row == rows_j[3])
        pick[pl.ds(base, 128), :] = jnp.where(hit, 1.0, 0.0).astype(BF16)

    @pl.loop(0, 24)
    def _(c):
        base = pl.multiple_of(c * 128, 128)
        col = lax.broadcasted_iota(I32, (128, 128), 1) + base
        for q in range(4):
            w = jnp.zeros((128, 128), F32)
            for j in range(4):
                w = w + jnp.where(col == r0s[:, j : j + 1] + 6 * q, rw_ref[:, j : j + 1], 0.0)
            hi = w.astype(BF16)
            whi[pl.ds(q * 128, 128), pl.ds(base, 128)] = hi
            wlo[pl.ds(q * 128, 128), pl.ds(base, 128)] = (w - hi.astype(F32)).astype(BF16)

    vext[:, 128:256] = jnp.ones((2048, 128), BF16)
    for i in range(15):
        landed(qkv_recv.at[0], qr_sem.at[i])
    vext[:, 0:128] = qkv_recv[:, 2].reshape(2048, 128)

    lam = lam_ref[0]
    coef = 0.125 * 1.4426950408889634

    def query_block(i):
        n = i + 1
        qb = qkv_recv[i, 0]
        lane = lax.broadcasted_iota(I32, (128, 128), 1)
        zero = jnp.zeros_like(qb)
        q2 = jnp.concatenate([jnp.where(lane < 64, qb, zero), jnp.where(lane >= 64, qb, zero)], axis=0)
        keys = qkv_recv[0:n, 1].reshape(n * 128, 128)
        s = lax.dot_general(q2, keys, (((1,), (1,)), ((), ())), preferred_element_type=F32)
        r2 = lax.broadcasted_iota(I32, (256, 128), 0) & 127
        c2 = lax.broadcasted_iota(I32, (256, 128), 1)
        diag = jnp.where(c2 <= r2, s[:, i * 128 :], -1e30)
        s = diag if i == 0 else jnp.concatenate([s[:, : i * 128], diag], axis=1)
        m = jnp.max(s, axis=1, keepdims=True)
        p = jnp.exp2((s - m) * coef).astype(BF16)
        ol = dot(p, vext[0 : n * 128, :])
        o = ol[:, 0:128] / ol[:, 128:256]
        return rms(o[0:128] - lam * o[128:256], hgain_ref[...]).astype(BF16)

    @pl.loop(0, 8)
    def _(j):
        a = lax.rem(sp + j, 8)
        for b in range(8):

            @pl.when(a == b)
            def _():
                head_send[b] = query_block(b)
                head_send[15 - b] = query_block(15 - b)

        for to in (a, 15 - a):

            @pl.when(to != sp)
            def _():
                pltpu.make_async_remote_copy(
                    head_send.at[to], head_recv.at[sp], hs_sem.at[to], hr_sem.at[sp],
                    device_id=(to, dp), device_id_type=MESH,
                ).start()

    head_recv[sp] = head_send[sp]

    loads[0].wait()
    own = jnp.where(sp < 8, sp, 15 - sp)
    acc[...] = jnp.zeros_like(acc)

    @pl.loop(0, 8)
    def _(j):
        h0 = lax.rem(own - j + 8, 8)
        for h in (h0, h0 + 8):

            @pl.when(h != sp)
            def _():
                landed(head_recv.at[h], hr_sem.at[h])

        x = jnp.concatenate([head_recv[h0], head_recv[h0 + 8]], axis=1)
        for c in range(4):
            cols = pl.ds(c * 512, 512)
            w = jnp.concatenate([wo[h0, :, cols], wo[h0 + 8, :, cols]], axis=0)
            acc[:, cols] += dot(x, w)

    updated = (res_ref[...].astype(F32) + rms(acc[...], mixg_ref[...])).astype(BF16)
    upd[...] = updated
    normed = rms(updated.astype(F32), preg_ref[...]).astype(BF16)
    for q in range(4):
        x4[q * 128 : (q + 1) * 128, :] = normed[:, q * 512 : (q + 1) * 512]

    for g in range(8):
        rows = dot(pick[g * 384 : (g + 1) * 384, :], x4[...]).astype(BF16)
        slab_send[g * 16 : (g + 1) * 16] = rows.reshape(16, 24, 512)
        for at in range(max(1, 16 * g), 16 * g + 16):
            pltpu.make_async_remote_copy(
                slab_send.at[at], slab_recv.at[at], ds_sem.at[0], dr_sem.at[at // 32],
                device_id=shifted(sp, dp, ALL_ORDER[at], 1), device_id_type=MESH,
            ).start()
    slab_recv[0] = slab_send[0]

    def hidden_of(x, wg, wu):
        gate, up = dot(x, wg), dot(x, wu)
        return (gate / (1.0 + jnp.exp(-gate)) * up).astype(BF16)

    for load in loads[1:]:
        load.wait()
    x4q = [x4[q * 128 : (q + 1) * 128, :] for q in range(4)]
    shared_h = hidden_of(jnp.concatenate(x4q, axis=1), sg[...], su[...])
    shared[...] = dot(shared_h, sd[...]).astype(BF16)

    @pl.loop(0, 4)
    def _(g):
        for gs in range(4):

            @pl.when(g == gs)
            def _():
                lo = max(1, 32 * gs)
                landed(slab_recv.at[pl.ds(lo, 32 * gs + 32 - lo)], dr_sem.at[gs])

        for b in range(4):
            block = slab_recv[pl.ds(g * 32 + b * 8, 8)].reshape(192, 512)
            y = dot(perm_ref[...], block).astype(BF16)
            for q in range(4):
                xs[b * 48 : (b + 1) * 48, q * 512 : (q + 1) * 512] = y[q * 48 : (q + 1) * 48]
        h = hidden_of(xs[...], eg[...], eu[...])
        xs[...] = dot(h, ed[...]).astype(BF16)
        for b in range(4):
            y = jnp.concatenate(
                [xs[b * 48 : (b + 1) * 48, q * 512 : (q + 1) * 512] for q in range(4)], axis=0
            )
            back = dot(permt_ref[...], y).astype(BF16)
            res_send[pl.ds(g * 32 + b * 8, 8)] = back.reshape(8, 24, 512)
        for gs in range(4):

            @pl.when(g == gs)
            def _():
                for at in range(max(1, 32 * gs), 32 * gs + 32):
                    pltpu.make_async_remote_copy(
                        res_send.at[at], res_recv.at[at], rs_sem.at[0], rr_sem.at[gs],
                        device_id=shifted(sp, dp, ALL_ORDER[at], -1), device_id_type=MESH,
                    ).start()

    res_recv[0] = res_send[0]

    mix = acc
    for g in range(4):
        lo = max(1, 32 * g)
        landed(res_recv.at[pl.ds(lo, 32 * g + 32 - lo)], rr_sem.at[g])
        rows = res_recv[g * 32 : (g + 1) * 32].reshape(768, 512)
        cols = pl.ds(g * 768, 768)
        for q in range(4):
            part = dot(whi[pl.ds(q * 128, 128), cols], rows) + dot(wlo[pl.ds(q * 128, 128), cols], rows)
            at = pl.ds(q * 512, 512)
            if g == 0:
                mix[:, at] = part
            else:
                mix[:, at] += part
    combined = mix[...] + shared[...].astype(F32)
    out_ref[...] = (upd[...].astype(F32) + rms(combined, postg_ref[...])).astype(BF16)

    for i in range(15):
        landed(qkv_send.at[0], qs_sem.at[i])
    for i in range(16):

        @pl.when(i != sp)
        def _():
            landed(head_send.at[i], hs_sem.at[i])

    landed(slab_send.at[pl.ds(1, 127)], ds_sem.at[0])
    landed(res_send.at[pl.ds(1, 127)], rs_sem.at[0])


def local(
    queries, key_vectors, value_vectors, head_lambda, head_gain, residual, out_weight, mix_gain, pre_gain,
    post_gain, routes, route_weights, expert_gate, expert_up, expert_down, shared_gate, shared_up, shared_down,
):
    order = np.zeros((8, 128), np.int32)
    order[:4] = np.array([digits(k) for k in ALL_ORDER]).T
    perm = np.zeros((192, 192), np.float32)
    for src in range(8):
        for q in range(4):
            for s in range(6):
                perm[q * 48 + src * 6 + s, src * 24 + q * 6 + s] = 1
    vm, hbm = pl.BlockSpec(memory_space=pltpu.VMEM), pl.BlockSpec(memory_space=pl.ANY)
    dma = pltpu.SemaphoreType.DMA
    slabs = pltpu.VMEM((128, 24, 512), BF16)
    out = pl.pallas_call(
        layer_kernel,
        out_shape=jax.ShapeDtypeStruct((128, 2048), BF16),
        in_specs=[vm, vm, vm, pl.BlockSpec(memory_space=pltpu.SMEM)] + [vm] * 10 + [hbm] * 7,
        out_specs=vm,
        scratch_shapes=[
            pltpu.VMEM((16, 128, 2048), BF16),
            pltpu.VMEM((2048, 512), BF16), pltpu.VMEM((2048, 512), BF16), pltpu.VMEM((512, 2048), BF16),
            pltpu.VMEM((2048, 512), BF16), pltpu.VMEM((2048, 512), BF16), pltpu.VMEM((512, 2048), BF16),
            pltpu.VMEM((3, 2048, 128), F32),
            pltpu.VMEM((16, 3, 128, 128), BF16), pltpu.VMEM((16, 3, 128, 128), BF16),
            pltpu.VMEM((2048, 256), BF16),
            pltpu.VMEM((16, 128, 128), BF16), pltpu.VMEM((16, 128, 128), BF16),
            pltpu.VMEM((128, 2048), F32),
            pltpu.VMEM((512, 512), BF16), pltpu.VMEM((3072, 512), BF16),
            slabs, slabs, slabs, slabs,
            pltpu.VMEM((512, 3072), BF16), pltpu.VMEM((512, 3072), BF16),
            pltpu.VMEM((192, 2048), BF16), pltpu.VMEM((128, 2048), BF16), pltpu.VMEM((128, 2048), BF16),
            pltpu.VMEM((128, 4), I32),
            dma((7,)), dma((15,)), dma((15,)), dma((16,)), dma((16,)), dma((1,)), dma((4,)), dma((1,)), dma((4,)),
        ],
        compiler_params=pltpu.CompilerParams(
            collective_id=0, has_side_effects=True, vmem_limit_bytes=67043328
        ),
    )(
        queries[0], key_vectors[0], value_vectors[0], head_lambda, head_gain.reshape(1, 128), residual[0],
        mix_gain.reshape(1, -1), pre_gain.reshape(1, -1), post_gain.reshape(1, -1), routes[0], route_weights[0],
        jnp.asarray(order), jnp.asarray(perm, BF16), jnp.asarray(perm.T, BF16),
        out_weight.reshape(16, 128, 2048), expert_gate[0], expert_up[0], expert_down[0],
        shared_gate, shared_up, shared_down,
    )
    return out.reshape(1, 128, 2048)


def solution(mesh):
    tokens, heads, experts = P("dp", "sp", None), P("dp", "sp", None, None), P(("sp", "dp"), None, None)
    return jax.shard_map(
        local,
        mesh=mesh,
        in_specs=(
            heads, heads, heads, P("sp"), P(), tokens, P(), P(), P(), P(), tokens, tokens,
            experts, experts, experts, P(), P(), P(),
        ),
        out_specs=tokens,
        check_vma=False,
    )
```

```python
import functools

import jax
import jax.numpy as jnp
import numpy as np
from jax import lax
from jax.experimental import pallas as pl
from jax.experimental.pallas import tpu as pltpu
from jax.sharding import PartitionSpec as P

MESH = pl.DeviceIdType.MESH
EPS = 1e-06
F32, BF16, I32 = jnp.float32, jnp.bfloat16, jnp.int32


def digits(k):
    return k // 32, (k // 8) % 4, (k // 2) % 4, k % 2


def link_load(k):
    load = np.zeros(6)
    dz, dy, dx, _ = digits(k)
    for i, d in enumerate((dx, dy, dz)):
        if d in (1, 2):
            load[2 * i] += 1
        if d in (2, 3):
            load[2 * i + 1] += 1
    return load


def first_link(k):
    dz, dy, dx, _ = digits(k)
    for i, d in enumerate((dx, dy, dz)):
        if d:
            return i, d
    return 3, 0


def balanced_order(offsets):
    left, total, out, last = list(offsets), np.zeros(6), [], None
    while left:

        def cost(k):
            t = total + link_load(k)
            return t.max() - t.min() + (0.5 if last is not None and first_link(k) == last else 0)

        k = min(left, key=cost)
        left.remove(k)
        out.append(k)
        total = total + link_load(k)
        last = first_link(k)
    return out


SP_ORDER = [k // 8 for k in balanced_order([8 * s for s in range(1, 16)])]
ALL_ORDER = [0] + balanced_order(range(1, 128))


def shifted(sp, dp, k, sign):
    dz, dy, dx, dc = digits(k)
    if sign < 0:
        dz, dy, dx, dc = -dz % 4, -dy % 4, -dx % 4, -dc % 2
    rem = lax.rem
    nsp = rem(sp // 4 + dz, 4) * 4 + rem(rem(sp, 4) + dy, 4)
    ndp = rem(dp // 2 + dx, 4) * 2 + rem(rem(dp, 2) + dc, 2)
    return nsp, ndp


def landed(ref, sem):
    pltpu.make_async_copy(ref, ref, sem).wait()


def dot(a, b):
    return jnp.dot(a, b, preferred_element_type=F32)


def rms(v, gain):
    return v * lax.rsqrt(jnp.mean(v * v, axis=-1, keepdims=True) + EPS) * gain


def layer_kernel(
    q_ref, k_ref, v_ref, lam_ref, hgain_ref, res_ref, mixg_ref, preg_ref, postg_ref,
    routes_ref, rw_ref, order_ref, perm_ref, permt_ref, turn_ref,
    wo_hbm, eg_hbm, eu_hbm, ed_hbm, sg_hbm, su_hbm, sd_hbm,
    out_ref,
    wo, wg, wu, wd,
    qkv_send, qkv_recv, p1, l1, mixture, head_send, head_recv, acc,
    x4, pick, slab_send, slab_recv, res_recv, xs, upd, shared, r0b, rwb,
    wsem, qs_sem, qr_sem, hs_sem, hr_sem, ds_sem, dr_sem, rs_sem, rr_sem, entered,
):
    sp, dp = lax.axis_index("sp"), lax.axis_index("dp")
    barrier = pltpu.get_barrier_semaphore()
    for d in range(1, 16):
        to, _ = shifted(sp, dp, 8 * d, 1)
        pl.semaphore_signal(barrier, inc=1, device_id=(to, dp), device_id_type=MESH)
    for d in range(1, 8):
        _, to = shifted(sp, dp, d, 1)
        pl.semaphore_signal(barrier, inc=1, device_id=(sp, to), device_id_type=MESH)

    def weights(i, src, dst):
        return pltpu.make_async_copy(src, dst, wsem.at[i])

    loads = [weights(0, wo_hbm, wo), weights(1, sg_hbm, wg), weights(2, su_hbm, wu), weights(3, sd_hbm, wd)]
    expert_loads = [weights(4, eg_hbm, wg), weights(5, eu_hbm, wu), weights(6, ed_hbm, wd)]

    turn = turn_ref[...]
    for g in range(8):
        at = slice(16 * g, 16 * (g + 1))
        q, k, v = (ref[at].reshape(256, 128) for ref in (q_ref, k_ref, v_ref))
        both = jnp.concatenate([q[:, :64], k[:, :64], q[:, 64:], k[:, 64:], v], axis=1)
        rows = dot(turn, both).astype(BF16)
        for part in range(3):
            qkv_send[part, :, at, :] = rows[:, part * 128 : (part + 1) * 128].reshape(16, 16, 128)
    pl.semaphore_wait(barrier, 22)
    for part in range(3):
        for i, d in enumerate(SP_ORDER):
            to, _ = shifted(sp, dp, 8 * d, 1)
            pltpu.make_async_remote_copy(
                qkv_send.at[part, to], qkv_recv.at[part, sp], qs_sem.at[part, i], qr_sem.at[part, i],
                device_id=(to, dp), device_id_type=MESH,
            ).start()
    for d in range(1, 8):
        _, to = shifted(sp, dp, d, 1)
        pl.semaphore_signal(entered, inc=1, device_id=(sp, to), device_id_type=MESH)
    for load in loads:
        load.start()
    for part in range(3):
        qkv_recv[part, sp] = qkv_send[part, sp]

    oz, oy, ox, oc = (order_ref[i : i + 1, :] for i in range(4))
    mz, my, mx, mc = sp // 4, lax.rem(sp, 4), dp // 2, lax.rem(dp, 2)
    expert = ((oz + mz) & 3) * 32 + ((oy + my) & 3) * 8 + ((ox + mx) & 3) * 2 + ((oc + mc) & 1)
    row_i = lax.broadcasted_iota(I32, (128, 128), 0)
    col_i = lax.broadcasted_iota(I32, (128, 128), 1)
    eye = col_i == row_i

    def as_column(row):
        return jnp.sum(jnp.where(eye, row, jnp.zeros_like(row)), axis=1, keepdims=True)

    hots = [as_column(routes_ref[j : j + 1, :].astype(F32)).astype(I32) == expert for j in range(4)]
    members = sum(h.astype(F32) for h in hots).astype(BF16)
    earlier = dot((col_i < row_i).astype(F32).astype(BF16), members)
    place = earlier + 24.0 * col_i.astype(F32)
    rows_j = []
    for j in range(4):
        r0 = jnp.sum(jnp.where(hots[j], place, 0.0), axis=1, keepdims=True)
        r0b[j] = jnp.broadcast_to(r0, (128, 128)).astype(I32)
        rwb[j] = jnp.broadcast_to(as_column(rw_ref[j : j + 1, :]), (128, 128))
        r0_row = jnp.sum(jnp.where(eye, r0, 0.0), axis=0, keepdims=True).astype(I32)
        rows_j.append(jnp.concatenate([r0_row + 6 * q for q in range(4)], axis=1))

    @pl.loop(0, 24)
    def _(c):
        base = pl.multiple_of(c * 128, 128)
        row = lax.broadcasted_iota(I32, (128, 512), 0) + base
        hit = (row == rows_j[0]) | (row == rows_j[1]) | (row == rows_j[2]) | (row == rows_j[3])
        pick[pl.ds(base, 128), :] = jnp.where(hit, 1.0, 0.0).astype(BF16)

    coef = 0.125 * 1.4426950408889634
    causal = lax.broadcasted_iota(I32, (256, 256), 1) <= lax.broadcasted_iota(I32, (256, 256), 0)

    def exponents(part, t):
        qk = qkv_recv[part, 2 * t : 2 * t + 2].reshape(256, 128)
        q = jnp.concatenate([jnp.zeros((256, 64), BF16), qk[:, :64]], axis=1)
        keys = qkv_recv[part, 0 : 2 * t + 2].reshape(256 * (t + 1), 128)
        s = lax.dot_general(q, keys, (((1,), (1,)), ((), ())), preferred_element_type=F32)
        diag = jnp.where(causal, s[:, t * 256 :], -1e30)
        s = diag if t == 0 else jnp.concatenate([s[:, : t * 256], diag], axis=1)
        p = jnp.exp2((s - jnp.max(s, axis=1, keepdims=True)) * coef)
        return p, jnp.sum(p, axis=1, keepdims=True)

    def tri(t):
        return t * (t + 1) // 2

    for i in range(15):
        landed(qkv_recv.at[0, 0], qr_sem.at[0, i])
    for t in range(8):
        p, l = exponents(0, t)
        l1[t] = jnp.broadcast_to(1.0 / l, (256, 128))
        for c in range(t + 1):
            p1[tri(t) + c] = p[:, c * 256 : (c + 1) * 256]
    for i in range(15):
        landed(qkv_recv.at[1, 0], qr_sem.at[1, i])
    lam = lam_ref[0]
    for t in range(8):
        p, l = exponents(1, t)
        scale1 = jnp.concatenate([l1[t], l1[t]], axis=1)
        scale2 = lam / l
        for c in range(t + 1):
            mixture[tri(t) + c] = (p1[tri(t) + c] * scale1 - p[:, c * 256 : (c + 1) * 256] * scale2).astype(BF16)
    for i in range(15):
        landed(qkv_recv.at[2, 0], qr_sem.at[2, i])
    for t in range(8):
        m = jnp.concatenate([mixture[tri(t) + c] for c in range(t + 1)], axis=1)
        o = dot(m, qkv_recv[2, 0 : 2 * t + 2].reshape(256 * (t + 1), 128))
        head_send[2 * t : 2 * t + 2] = rms(o, hgain_ref[...]).astype(BF16).reshape(2, 128, 128)
    for i, d in enumerate(SP_ORDER):
        to, _ = shifted(sp, dp, 8 * d, 1)
        pltpu.make_async_remote_copy(
            head_send.at[to], head_recv.at[sp], hs_sem.at[i], hr_sem.at[i],
            device_id=(to, dp), device_id_type=MESH,
        ).start()
    head_recv[sp] = head_send[sp]

    loads[0].wait()
    sources = [sp] + [shifted(sp, dp, 8 * d, -1)[0] for d in SP_ORDER]
    for i in range(0, 16, 2):
        for n in (i, i + 1):
            if n:
                landed(head_recv.at[0], hr_sem.at[n - 1])
        h0, h1 = sources[i], sources[i + 1]
        x = jnp.concatenate([head_recv[h0], head_recv[h1]], axis=1)
        for c in range(4):
            cols = pl.ds(c * 512, 512)
            part = dot(x, jnp.concatenate([wo[h0, :, cols], wo[h1, :, cols]], axis=0))
            if i == 0:
                acc[:, cols] = part
            else:
                acc[:, cols] += part

    updated = (res_ref[...].astype(F32) + rms(acc[...], mixg_ref[...])).astype(BF16)
    upd[...] = updated
    normed = rms(updated.astype(F32), preg_ref[...]).astype(BF16)
    for q in range(4):
        x4[q * 128 : (q + 1) * 128, :] = normed[:, q * 512 : (q + 1) * 512]

    pl.semaphore_wait(entered, 7)
    for g in range(8):
        rows = dot(pick[g * 384 : (g + 1) * 384, :], x4[...]).astype(BF16)
        slab_send[g * 16 : (g + 1) * 16] = rows.reshape(16, 24, 512)
        for at in range(max(1, 16 * g), 16 * g + 16):
            pltpu.make_async_remote_copy(
                slab_send.at[at], slab_recv.at[at], ds_sem.at[0], dr_sem.at[at // 32],
                device_id=shifted(sp, dp, ALL_ORDER[at], 1), device_id_type=MESH,
            ).start()
    slab_recv[0] = slab_send[0]

    def hidden_of(x):
        gate, up = dot(x, wg[...]), dot(x, wu[...])
        return (gate / (1.0 + jnp.exp(-gate)) * up).astype(BF16)

    for load in loads[1:]:
        load.wait()
    shared_h = hidden_of(jnp.concatenate([x4[q * 128 : (q + 1) * 128, :] for q in range(4)], axis=1))
    shared[...] = dot(shared_h, wd[...]).astype(BF16)
    for load in expert_loads:
        load.start()

    @pl.loop(0, 12)
    def _(c):
        for half in range(2):
            col = lax.broadcasted_iota(I32, (128, 128), 1) + (c * 256 + half * 128)
            for q in range(4):
                w = jnp.zeros((128, 128), F32)
                for j in range(4):
                    w = jnp.where(col == r0b[j] + 6 * q, rwb[j], w)
                p1[(q // 2) * 12 + c, pl.ds((q % 2) * 128, 128), pl.ds(half * 128, 128)] = w

    for load in expert_loads:
        load.wait()

    @pl.loop(0, 4)
    def _(g):
        for gs in range(4):

            @pl.when(g == gs)
            def _():
                lo = max(1, 32 * gs)
                landed(slab_recv.at[pl.ds(lo, 32 * gs + 32 - lo)], dr_sem.at[gs])

        for b in range(4):
            block = slab_recv[pl.ds(g * 32 + b * 8, 8)].reshape(192, 512)
            y = dot(perm_ref[...], block).astype(BF16)
            for q in range(4):
                xs[b * 48 : (b + 1) * 48, q * 512 : (q + 1) * 512] = y[q * 48 : (q + 1) * 48]
        h = hidden_of(xs[...])
        xs[...] = dot(h, wd[...]).astype(BF16)
        for b in range(4):
            y = jnp.concatenate(
                [xs[b * 48 : (b + 1) * 48, q * 512 : (q + 1) * 512] for q in range(4)], axis=0
            )
            back = dot(permt_ref[...], y).astype(BF16)
            slab_recv[pl.ds(g * 32 + b * 8, 8)] = back.reshape(8, 24, 512)
        for gs in range(4):

            @pl.when(g == gs)
            def _():
                for at in range(max(1, 32 * gs), 32 * gs + 32):
                    pltpu.make_async_remote_copy(
                        slab_recv.at[at], res_recv.at[at], rs_sem.at[0], rr_sem.at[gs],
                        device_id=shifted(sp, dp, ALL_ORDER[at], -1), device_id_type=MESH,
                    ).start()

    res_recv[0] = slab_recv[0]

    for g in range(4):
        lo = max(1, 32 * g)
        landed(res_recv.at[pl.ds(lo, 32 * g + 32 - lo)], rr_sem.at[g])
        rows = res_recv[g * 32 : (g + 1) * 32].reshape(768, 512)
        for qq in range(2):
            w = jnp.concatenate([p1[qq * 12 + 3 * g + c] for c in range(3)], axis=1)
            hi = w.astype(BF16)
            part = dot(hi, rows) + dot((w - hi.astype(F32)).astype(BF16), rows)
            for q in range(2):
                at = pl.ds((2 * qq + q) * 512, 512)
                if g == 0:
                    acc[:, at] = part[q * 128 : (q + 1) * 128]
                else:
                    acc[:, at] += part[q * 128 : (q + 1) * 128]
    combined = acc[...] + shared[...].astype(F32)
    out_ref[...] = (upd[...].astype(F32) + rms(combined, postg_ref[...])).astype(BF16)

    for i in range(15):
        for part in range(3):
            landed(qkv_send.at[part, 0], qs_sem.at[part, i])
        landed(head_send.at[0], hs_sem.at[i])
    landed(slab_send.at[pl.ds(1, 127)], ds_sem.at[0])
    landed(slab_recv.at[pl.ds(1, 127)], rs_sem.at[0])


def local(
    queries, key_vectors, value_vectors, head_lambda, head_gain, residual, out_weight, mix_gain, pre_gain,
    post_gain, routes, route_weights, expert_gate, expert_up, expert_down, shared_gate, shared_up, shared_down,
):
    order = np.zeros((8, 128), np.int32)
    order[:4] = np.array([digits(k) for k in ALL_ORDER]).T
    perm = np.zeros((192, 192), np.float32)
    for src in range(8):
        for q in range(4):
            for s in range(6):
                perm[q * 48 + src * 6 + s, src * 24 + q * 6 + s] = 1
    turn = np.zeros((256, 256), np.float32)
    for h in range(16):
        for t in range(16):
            turn[h * 16 + t, t * 16 + h] = 1
    vm, hbm = pl.BlockSpec(memory_space=pltpu.VMEM), pl.BlockSpec(memory_space=pl.ANY)
    dma = pltpu.SemaphoreType.DMA
    slabs = pltpu.VMEM((128, 24, 512), BF16)
    out = pl.pallas_call(
        layer_kernel,
        out_shape=jax.ShapeDtypeStruct((128, 2048), BF16),
        in_specs=[vm, vm, vm, pl.BlockSpec(memory_space=pltpu.SMEM)] + [vm] * 11 + [hbm] * 7,
        out_specs=vm,
        scratch_shapes=[
            pltpu.VMEM((16, 128, 2048), BF16),
            pltpu.VMEM((2048, 512), BF16), pltpu.VMEM((2048, 512), BF16), pltpu.VMEM((512, 2048), BF16),
            pltpu.VMEM((3, 16, 128, 128), BF16), pltpu.VMEM((3, 16, 128, 128), BF16),
            pltpu.VMEM((36, 256, 256), F32), pltpu.VMEM((8, 256, 128), F32), pltpu.VMEM((36, 256, 256), BF16),
            pltpu.VMEM((16, 128, 128), BF16), pltpu.VMEM((16, 128, 128), BF16),
            pltpu.VMEM((128, 2048), F32),
            pltpu.VMEM((512, 512), BF16), pltpu.VMEM((3072, 512), BF16),
            slabs, slabs, slabs,
            pltpu.VMEM((192, 2048), BF16), pltpu.VMEM((128, 2048), BF16), pltpu.VMEM((128, 2048), BF16),
            pltpu.VMEM((4, 128, 128), I32), pltpu.VMEM((4, 128, 128), F32),
            dma((7,)), dma((3, 15)), dma((3, 15)), dma((15,)), dma((15,)), dma((1,)), dma((4,)), dma((1,)), dma((4,)),
            pltpu.SemaphoreType.REGULAR,
        ],
        compiler_params=pltpu.CompilerParams(
            collective_id=0, has_side_effects=True, vmem_limit_bytes=67043328
        ),
    )(
        queries[0], key_vectors[0], value_vectors[0], head_lambda, head_gain.reshape(1, 128), residual[0],
        mix_gain.reshape(1, -1), pre_gain.reshape(1, -1), post_gain.reshape(1, -1), routes[0].T, route_weights[0].T,
        jnp.asarray(order), jnp.asarray(perm, BF16), jnp.asarray(perm.T, BF16), jnp.asarray(turn, BF16),
        out_weight.reshape(16, 128, 2048), expert_gate[0], expert_up[0], expert_down[0],
        shared_gate, shared_up, shared_down,
    )
    return out.reshape(1, 128, 2048)


def solution(mesh):
    tokens, heads, experts = P("dp", "sp", None), P("dp", "sp", None, None), P(("sp", "dp"), None, None)
    return jax.shard_map(
        local,
        mesh=mesh,
        in_specs=(
            heads, heads, heads, P("sp"), P(), tokens, P(), P(), P(), P(), tokens, tokens,
            experts, experts, experts, P(), P(), P(),
        ),
        out_specs=tokens,
        check_vma=False,
    )
```

```python
import jax
import jax.numpy as jnp
import numpy as np
from jax import lax
from jax.experimental import pallas as pl
from jax.experimental.pallas import tpu as pltpu
from jax.sharding import PartitionSpec as P

MESH = pl.DeviceIdType.MESH
EPS = 1e-06
F32, BF16, I32 = jnp.float32, jnp.bfloat16, jnp.int32


def digits(k):
    return k // 32, (k // 8) % 4, (k // 2) % 4, k % 2


def link_load(k):
    load = np.zeros(6)
    dz, dy, dx, _ = digits(k)
    for i, d in enumerate((dx, dy, dz)):
        if d in (1, 2):
            load[2 * i] += 1
        if d in (2, 3):
            load[2 * i + 1] += 1
    return load


def first_link(k):
    dz, dy, dx, _ = digits(k)
    for i, d in enumerate((dx, dy, dz)):
        if d:
            return i, d
    return 3, 0


def balanced_order(offsets):
    left, total, out, last = list(offsets), np.zeros(6), [], None
    while left:

        def cost(k):
            t = total + link_load(k)
            return t.max() - t.min() + (0.5 if last is not None and first_link(k) == last else 0)

        k = min(left, key=cost)
        left.remove(k)
        out.append(k)
        total = total + link_load(k)
        last = first_link(k)
    return out


SP_ORDER = [k // 8 for k in balanced_order([8 * s for s in range(1, 16)])]
ALL_ORDER = [0] + balanced_order(range(1, 128))


class Peers:
    def __init__(self, sp, dp):
        rem = lax.rem
        z, y, x, c = sp // 4, rem(sp, 4), dp // 2, rem(dp, 2)
        self.z = [4 * z] + [4 * rem(z + i, 4) for i in (1, 2, 3)]
        self.y = [y] + [rem(y + i, 4) for i in (1, 2, 3)]
        self.x = [2 * x] + [2 * rem(x + i, 4) for i in (1, 2, 3)]
        self.c = [c, 1 - c]

    def at(self, k, sign=1):
        dz, dy, dx, dc = digits(k)
        if sign < 0:
            dz, dy, dx = -dz % 4, -dy % 4, -dx % 4
        return self.z[dz] + self.y[dy], self.x[dx] + self.c[dc]

    def sp(self, d, sign=1):
        return self.at(8 * d, sign)[0]


def landed(ref, sem):
    pltpu.make_async_copy(ref, ref, sem).wait()


def dot(a, b):
    return jnp.dot(a, b, preferred_element_type=F32)


def rms(v, gain):
    return v * lax.rsqrt(jnp.mean(v * v, axis=-1, keepdims=True) + EPS) * gain


def layer_kernel(
    lam_ref,
    q_hbm, k_hbm, v_hbm, hgain_hbm, res_hbm, mixg_hbm, preg_hbm, postg_hbm,
    routes_hbm, rw_hbm, order_hbm, perm_hbm, permt_hbm, turn_hbm,
    wo_hbm, eg_hbm, eu_hbm, ed_hbm, sg_hbm, su_hbm, sd_hbm,
    out_ref,
    q_ref, k_ref, v_ref, hgain_ref, res_ref, mixg_ref, preg_ref, postg_ref,
    routes_ref, rw_ref, order_ref, perm_ref, permt_ref, turn_ref,
    wo, wg, wu, wd,
    qkv_send, qkv_recv, p1, l1, mixture, head_send, head_recv, acc,
    x4, pick, slab_send, slab_recv, res_recv, xs, shared, r0b, rwb,
    wsem, isem, qs_sem, qr_sem, hs_sem, hr_sem, ds_sem, dr_sem, rs_sem, rr_sem, entered,
):
    sp, dp = lax.axis_index("sp"), lax.axis_index("dp")
    peers = Peers(sp, dp)
    barrier = pltpu.get_barrier_semaphore()
    for k in [8 * d for d in range(1, 16)] + list(range(1, 8)):
        pl.semaphore_signal(barrier, inc=1, device_id=peers.at(k), device_id_type=MESH)
    inputs = [
        pltpu.make_async_copy(src, dst, isem.at[i])
        for i, (src, dst) in enumerate(
            (
                (q_hbm, q_ref), (k_hbm, k_ref), (v_hbm, v_ref), (turn_hbm, turn_ref),
                (routes_hbm, routes_ref), (rw_hbm, rw_ref), (order_hbm, order_ref),
                (hgain_hbm, hgain_ref), (res_hbm, res_ref), (mixg_hbm, mixg_ref), (preg_hbm, preg_ref),
                (postg_hbm, postg_ref), (perm_hbm, perm_ref), (permt_hbm, permt_ref),
            )
        )
    ]
    for load in inputs:
        load.start()

    def weights(i, src, dst):
        return pltpu.make_async_copy(src, dst, wsem.at[i])

    loads = [weights(0, wo_hbm, wo), weights(1, sg_hbm, wg), weights(2, su_hbm, wu), weights(3, sd_hbm, wd)]
    expert_loads = [weights(4, eg_hbm, wg), weights(5, eu_hbm, wu), weights(6, ed_hbm, wd)]

    for load in inputs[:4]:
        load.wait()
    turn = turn_ref[...]
    for g in range(8):
        at = slice(16 * g, 16 * (g + 1))
        q, k, v = (ref[at].reshape(256, 128) for ref in (q_ref, k_ref, v_ref))
        both = jnp.concatenate([q[:, :64], k[:, :64], q[:, 64:], k[:, 64:], v], axis=1)
        rows = dot(turn, both).astype(BF16)
        for part in range(3):
            qkv_send[part, :, at, :] = rows[:, part * 128 : (part + 1) * 128].reshape(16, 16, 128)
    pl.semaphore_wait(barrier, 22)
    for part in range(3):
        for i, d in enumerate(SP_ORDER):
            to = peers.sp(d)
            pltpu.make_async_remote_copy(
                qkv_send.at[part, to], qkv_recv.at[part, sp], qs_sem.at[part, i], qr_sem.at[part, i],
                device_id=(to, dp), device_id_type=MESH,
            ).start()
    for d in range(1, 8):
        pl.semaphore_signal(entered, inc=1, device_id=peers.at(d), device_id_type=MESH)
    for load in loads:
        load.start()
    for part in range(3):
        qkv_recv[part, sp] = qkv_send[part, sp]

    for load in inputs[4:]:
        load.wait()
    oz, oy, ox, oc = (order_ref[i : i + 1, :] for i in range(4))
    mz, my, mx, mc = sp // 4, lax.rem(sp, 4), dp // 2, lax.rem(dp, 2)
    expert = ((oz + mz) & 3) * 32 + ((oy + my) & 3) * 8 + ((ox + mx) & 3) * 2 + ((oc + mc) & 1)
    row_i = lax.broadcasted_iota(I32, (128, 128), 0)
    col_i = lax.broadcasted_iota(I32, (128, 128), 1)
    eye = col_i == row_i

    def as_column(row):
        return jnp.sum(jnp.where(eye, row, jnp.zeros_like(row)), axis=1, keepdims=True)

    hots = [as_column(routes_ref[j : j + 1, :].astype(F32)).astype(I32) == expert for j in range(4)]
    members = sum(h.astype(F32) for h in hots).astype(BF16)
    earlier = dot((col_i < row_i).astype(F32).astype(BF16), members)
    place = earlier + 24.0 * col_i.astype(F32)
    rows_j = []
    for j in range(4):
        r0 = jnp.sum(jnp.where(hots[j], place, 0.0), axis=1, keepdims=True)
        r0b[j] = jnp.broadcast_to(r0, (128, 128)).astype(I32)
        rwb[j] = jnp.broadcast_to(as_column(rw_ref[j : j + 1, :]), (128, 128))
        r0_row = jnp.sum(jnp.where(eye, r0, 0.0), axis=0, keepdims=True).astype(I32)
        rows_j.append(jnp.concatenate([r0_row + 6 * q for q in range(4)], axis=1))

    @pl.loop(0, 24)
    def _(c):
        base = pl.multiple_of(c * 128, 128)
        row = lax.broadcasted_iota(I32, (128, 512), 0) + base
        hit = (row == rows_j[0]) | (row == rows_j[1]) | (row == rows_j[2]) | (row == rows_j[3])
        pick[pl.ds(base, 128), :] = jnp.where(hit, 1.0, 0.0).astype(BF16)

    coef = 0.125 * 1.4426950408889634
    causal = lax.broadcasted_iota(I32, (256, 256), 1) <= lax.broadcasted_iota(I32, (256, 256), 0)

    def exponents(part, t):
        qk = qkv_recv[part, 2 * t : 2 * t + 2].reshape(256, 128)
        q = jnp.concatenate([jnp.zeros((256, 64), BF16), qk[:, :64]], axis=1)
        keys = qkv_recv[part, 0 : 2 * t + 2].reshape(256 * (t + 1), 128)
        s = lax.dot_general(q, keys, (((1,), (1,)), ((), ())), preferred_element_type=F32)
        diag = jnp.where(causal, s[:, t * 256 :], -1e30)
        s = diag if t == 0 else jnp.concatenate([s[:, : t * 256], diag], axis=1)
        p = jnp.exp2((s - jnp.max(s, axis=1, keepdims=True)) * coef)
        return p, jnp.sum(p, axis=1, keepdims=True)

    def tri(t):
        return t * (t + 1) // 2

    for i in range(15):
        landed(qkv_recv.at[0, 0], qr_sem.at[0, i])
    for t in range(8):
        p, l = exponents(0, t)
        l1[t] = jnp.broadcast_to(1.0 / l, (256, 128))
        for c in range(t + 1):
            p1[tri(t) + c] = p[:, c * 256 : (c + 1) * 256]
    for i in range(15):
        landed(qkv_recv.at[1, 0], qr_sem.at[1, i])
    lam = lam_ref[0]
    for t in range(8):
        p, l = exponents(1, t)
        scale1 = jnp.concatenate([l1[t], l1[t]], axis=1)
        scale2 = lam / l
        for c in range(t + 1):
            mixture[tri(t) + c] = (p1[tri(t) + c] * scale1 - p[:, c * 256 : (c + 1) * 256] * scale2).astype(BF16)
    for i in range(15):
        landed(qkv_recv.at[2, 0], qr_sem.at[2, i])
    for t in range(8):
        m = jnp.concatenate([mixture[tri(t) + c] for c in range(t + 1)], axis=1)
        o = dot(m, qkv_recv[2, 0 : 2 * t + 2].reshape(256 * (t + 1), 128))
        head_send[2 * t : 2 * t + 2] = rms(o, hgain_ref[...]).astype(BF16).reshape(2, 128, 128)
    for i, d in enumerate(SP_ORDER):
        to = peers.sp(d)
        pltpu.make_async_remote_copy(
            head_send.at[to], head_recv.at[sp], hs_sem.at[i + 1], hr_sem.at[i + 1],
            device_id=(to, dp), device_id_type=MESH,
        ).start()
    head_recv[sp] = head_send[sp]

    loads[0].wait()
    sources = [sp] + [peers.sp(d, -1) for d in SP_ORDER]
    for i in range(0, 16, 2):
        for n in (i, i + 1):
            if n:
                landed(head_recv.at[0], hr_sem.at[n])
        h0, h1 = sources[i], sources[i + 1]
        x = jnp.concatenate([head_recv[h0], head_recv[h1]], axis=1)
        for c in range(4):
            cols = pl.ds(c * 512, 512)
            part = dot(x, jnp.concatenate([wo[h0, :, cols], wo[h1, :, cols]], axis=0))
            if i == 0:
                acc[:, cols] = part
            else:
                acc[:, cols] += part

    updated = (res_ref[...].astype(F32) + rms(acc[...], mixg_ref[...])).astype(BF16)
    res_ref[...] = updated
    normed = rms(updated.astype(F32), preg_ref[...]).astype(BF16)
    for q in range(4):
        x4[q * 128 : (q + 1) * 128, :] = normed[:, q * 512 : (q + 1) * 512]

    pl.semaphore_wait(entered, 7)
    for g in range(8):
        rows = dot(pick[g * 384 : (g + 1) * 384, :], x4[...]).astype(BF16)
        slab_send[g * 16 : (g + 1) * 16] = rows.reshape(16, 24, 512)
        for at in range(max(1, 16 * g), 16 * g + 16):
            pltpu.make_async_remote_copy(
                slab_send.at[at], slab_recv.at[at], ds_sem.at[0], dr_sem.at[at // 32],
                device_id=peers.at(ALL_ORDER[at]), device_id_type=MESH,
            ).start()
    slab_recv[0] = slab_send[0]

    def hidden_of(x):
        gate, up = dot(x, wg[...]), dot(x, wu[...])
        return (gate / (1.0 + jnp.exp(-gate)) * up).astype(BF16)

    for load in loads[1:]:
        load.wait()
    shared_h = hidden_of(jnp.concatenate([x4[q * 128 : (q + 1) * 128, :] for q in range(4)], axis=1))
    shared[...] = dot(shared_h, wd[...]).astype(BF16)
    for load in expert_loads:
        load.start()

    @pl.loop(0, 12)
    def _(c):
        for half in range(2):
            col = lax.broadcasted_iota(I32, (128, 128), 1) + (c * 256 + half * 128)
            for q in range(4):
                w = jnp.zeros((128, 128), F32)
                for j in range(4):
                    w = jnp.where(col == r0b[j] + 6 * q, rwb[j], w)
                p1[(q // 2) * 12 + c, pl.ds((q % 2) * 128, 128), pl.ds(half * 128, 128)] = w

    for load in expert_loads:
        load.wait()
    for i in range(15):
        for part in range(3):
            landed(qkv_send.at[part, 0], qs_sem.at[part, i])
        landed(head_send.at[0], hs_sem.at[i + 1])

    @pl.loop(0, 4)
    def _(g):
        for gs in range(4):

            @pl.when(g == gs)
            def _():
                lo = max(1, 32 * gs)
                landed(slab_recv.at[pl.ds(lo, 32 * gs + 32 - lo)], dr_sem.at[gs])

        for b in range(4):
            block = slab_recv[pl.ds(g * 32 + b * 8, 8)].reshape(192, 512)
            y = dot(perm_ref[...], block).astype(BF16)
            for q in range(4):
                xs[b * 48 : (b + 1) * 48, q * 512 : (q + 1) * 512] = y[q * 48 : (q + 1) * 48]
        h = hidden_of(xs[...])
        xs[...] = dot(h, wd[...]).astype(BF16)
        for b in range(4):
            y = jnp.concatenate(
                [xs[b * 48 : (b + 1) * 48, q * 512 : (q + 1) * 512] for q in range(4)], axis=0
            )
            back = dot(permt_ref[...], y).astype(BF16)
            slab_recv[pl.ds(g * 32 + b * 8, 8)] = back.reshape(8, 24, 512)
        for gs in range(4):

            @pl.when(g == gs)
            def _():
                for at in range(max(1, 32 * gs), 32 * gs + 32):
                    pltpu.make_async_remote_copy(
                        slab_recv.at[at], res_recv.at[at], rs_sem.at[0], rr_sem.at[at // 16],
                        device_id=peers.at(ALL_ORDER[at], -1), device_id_type=MESH,
                    ).start()

    res_recv[0] = slab_recv[0]

    for u in range(8):
        lo = max(1, 16 * u)
        landed(res_recv.at[pl.ds(lo, 16 * u + 16 - lo)], rr_sem.at[u])
        rows = res_recv[u * 16 : (u + 1) * 16].reshape(384, 512)
        for qq in range(2):
            blocks = [divmod(3 * u + c, 2) for c in range(3)]
            w = jnp.concatenate(
                [p1[qq * 12 + b, :, half * 128 : (half + 1) * 128] for b, half in blocks], axis=1
            )
            hi = w.astype(BF16)
            part = dot(hi, rows) + dot((w - hi.astype(F32)).astype(BF16), rows)
            for q in range(2):
                at = pl.ds((2 * qq + q) * 512, 512)
                if u == 0:
                    acc[:, at] = part[q * 128 : (q + 1) * 128]
                else:
                    acc[:, at] += part[q * 128 : (q + 1) * 128]
    combined = acc[...] + shared[...].astype(F32)
    out_ref[...] = (res_ref[...].astype(F32) + rms(combined, postg_ref[...])).astype(BF16)

    landed(slab_send.at[pl.ds(1, 127)], ds_sem.at[0])
    landed(slab_recv.at[pl.ds(1, 127)], rs_sem.at[0])


def local(
    queries, key_vectors, value_vectors, head_lambda, head_gain, residual, out_weight, mix_gain, pre_gain,
    post_gain, routes, route_weights, expert_gate, expert_up, expert_down, shared_gate, shared_up, shared_down,
):
    order = np.zeros((8, 128), np.int32)
    order[:4] = np.array([digits(k) for k in ALL_ORDER]).T
    perm = np.zeros((192, 192), np.float32)
    for src in range(8):
        for q in range(4):
            for s in range(6):
                perm[q * 48 + src * 6 + s, src * 24 + q * 6 + s] = 1
    turn = np.zeros((256, 256), np.float32)
    for h in range(16):
        for t in range(16):
            turn[h * 16 + t, t * 16 + h] = 1
    vm, hbm = pl.BlockSpec(memory_space=pltpu.VMEM), pl.BlockSpec(memory_space=pl.ANY)
    dma = pltpu.SemaphoreType.DMA
    slabs = pltpu.VMEM((128, 24, 512), BF16)
    heads, wide = pltpu.VMEM((128, 16, 128), BF16), pltpu.VMEM((1, 2048), F32)
    out = pl.pallas_call(
        layer_kernel,
        out_shape=jax.ShapeDtypeStruct((128, 2048), BF16),
        in_specs=[pl.BlockSpec(memory_space=pltpu.SMEM)] + [hbm] * 21,
        out_specs=vm,
        scratch_shapes=[
            heads, heads, heads, pltpu.VMEM((1, 128), F32), pltpu.VMEM((128, 2048), BF16),
            wide, wide, wide, pltpu.VMEM((4, 128), I32), pltpu.VMEM((4, 128), F32), pltpu.VMEM((8, 128), I32),
            pltpu.VMEM((192, 192), BF16), pltpu.VMEM((192, 192), BF16), pltpu.VMEM((256, 256), BF16),
            pltpu.VMEM((16, 128, 2048), BF16),
            pltpu.VMEM((2048, 512), BF16), pltpu.VMEM((2048, 512), BF16), pltpu.VMEM((512, 2048), BF16),
            pltpu.VMEM((3, 16, 128, 128), BF16), pltpu.VMEM((3, 16, 128, 128), BF16),
            pltpu.VMEM((36, 256, 256), F32), pltpu.VMEM((8, 256, 128), F32), pltpu.VMEM((36, 256, 256), BF16),
            pltpu.VMEM((16, 128, 128), BF16), pltpu.VMEM((16, 128, 128), BF16),
            pltpu.VMEM((128, 2048), F32),
            pltpu.VMEM((512, 512), BF16), pltpu.VMEM((3072, 512), BF16),
            slabs, slabs, slabs,
            pltpu.VMEM((192, 2048), BF16), pltpu.VMEM((128, 2048), BF16),
            pltpu.VMEM((4, 128, 128), I32), pltpu.VMEM((4, 128, 128), F32),
            dma((7,)), dma((14,)), dma((3, 15)), dma((3, 15)), dma((16,)), dma((16,)), dma((1,)), dma((4,)), dma((1,)), dma((8,)),
            pltpu.SemaphoreType.REGULAR,
        ],
        compiler_params=pltpu.CompilerParams(
            collective_id=0, has_side_effects=True, vmem_limit_bytes=67043328
        ),
    )(
        head_lambda, queries[0], key_vectors[0], value_vectors[0], head_gain.reshape(1, 128), residual[0],
        mix_gain.reshape(1, -1), pre_gain.reshape(1, -1), post_gain.reshape(1, -1), routes[0].T, route_weights[0].T,
        jnp.asarray(order), jnp.asarray(perm, BF16), jnp.asarray(perm.T, BF16), jnp.asarray(turn, BF16),
        out_weight.reshape(16, 128, 2048), expert_gate[0], expert_up[0], expert_down[0],
        shared_gate, shared_up, shared_down,
    )
    return out.reshape(1, 128, 2048)


def solution(mesh):
    tokens, heads, experts = P("dp", "sp", None), P("dp", "sp", None, None), P(("sp", "dp"), None, None)
    return jax.shard_map(
        local,
        mesh=mesh,
        in_specs=(
            heads, heads, heads, P("sp"), P(), tokens, P(), P(), P(), P(), tokens, tokens,
            experts, experts, experts, P(), P(), P(),
        ),
        out_specs=tokens,
        check_vma=False,
    )
```

```python
import jax
import jax.numpy as jnp
import numpy as np
from jax import lax
from jax.experimental import pallas as pl
from jax.experimental.pallas import tpu as pltpu
from jax.sharding import PartitionSpec as P

MESH = pl.DeviceIdType.MESH
EPS = 1e-06
F32, BF16, I32 = jnp.float32, jnp.bfloat16, jnp.int32


def digits(k):
    return k // 32, (k // 8) % 4, (k // 2) % 4, k % 2


def link_load(k):
    load = np.zeros(6)
    dz, dy, dx, _ = digits(k)
    for i, d in enumerate((dx, dy, dz)):
        if d in (1, 2):
            load[2 * i] += 1
        if d in (2, 3):
            load[2 * i + 1] += 1
    return load


def first_link(k):
    dz, dy, dx, _ = digits(k)
    for i, d in enumerate((dx, dy, dz)):
        if d:
            return i, d
    return 3, 0


def balanced_order(offsets):
    left, total, out, last = list(offsets), np.zeros(6), [], None
    while left:

        def cost(k):
            t = total + link_load(k)
            return t.max() - t.min() + (0.5 if last is not None and first_link(k) == last else 0)

        k = min(left, key=cost)
        left.remove(k)
        out.append(k)
        total = total + link_load(k)
        last = first_link(k)
    return out


SP_ORDER = [k // 8 for k in balanced_order([8 * s for s in range(1, 16)])]
ALL_ORDER = [0] + [int(v) for v in np.random.RandomState(4).permutation(np.arange(1, 128))]


class Peers:
    def __init__(self, sp, dp):
        rem = lax.rem
        z, y, x, c = sp // 4, rem(sp, 4), dp // 2, rem(dp, 2)
        self.z = [4 * z] + [4 * rem(z + i, 4) for i in (1, 2, 3)]
        self.y = [y] + [rem(y + i, 4) for i in (1, 2, 3)]
        self.x = [2 * x] + [2 * rem(x + i, 4) for i in (1, 2, 3)]
        self.c = [c, 1 - c]

    def at(self, k, sign=1):
        dz, dy, dx, dc = digits(k)
        if sign < 0:
            dz, dy, dx = -dz % 4, -dy % 4, -dx % 4
        return self.z[dz] + self.y[dy], self.x[dx] + self.c[dc]

    def sp(self, d, sign=1):
        return self.at(8 * d, sign)[0]


def landed(ref, sem):
    pltpu.make_async_copy(ref, ref, sem).wait()


def dot(a, b):
    return jnp.dot(a, b, preferred_element_type=F32)


def rms(v, gain):
    return v * lax.rsqrt(jnp.mean(v * v, axis=-1, keepdims=True) + EPS) * gain


def layer_kernel(
    lam_ref,
    q_hbm, k_hbm, v_hbm, hgain_hbm, res_hbm, mixg_hbm, preg_hbm, postg_hbm,
    routes_hbm, rw_hbm, order_hbm, perm_hbm, permt_hbm, turn_hbm,
    wo_hbm, eg_hbm, eu_hbm, ed_hbm, sg_hbm, su_hbm, sd_hbm,
    out_ref,
    q_ref, k_ref, v_ref, hgain_ref, res_ref, mixg_ref, preg_ref, postg_ref,
    routes_ref, rw_ref, order_ref, perm_ref, permt_ref, turn_ref,
    wo, wg, wu, wd,
    qkv_send, qkv_recv, p1, l1, mixture, head_send, head_recv, acc,
    x4, pick, slab_send, slab_recv, res_recv, xs, shared, r0b, rwb,
    wsem, isem, qs_sem, qr_sem, hs_sem, hr_sem, ds_sem, dr_sem, rs_sem, rr_sem, entered,
):
    sp, dp = lax.axis_index("sp"), lax.axis_index("dp")
    peers = Peers(sp, dp)
    barrier = pltpu.get_barrier_semaphore()
    for k in [8 * d for d in range(1, 16)] + list(range(1, 8)):
        pl.semaphore_signal(barrier, inc=1, device_id=peers.at(k), device_id_type=MESH)
    inputs = [
        pltpu.make_async_copy(src, dst, isem.at[i])
        for i, (src, dst) in enumerate(
            (
                (q_hbm, q_ref), (k_hbm, k_ref), (v_hbm, v_ref), (turn_hbm, turn_ref),
                (routes_hbm, routes_ref), (rw_hbm, rw_ref), (order_hbm, order_ref),
                (hgain_hbm, hgain_ref), (res_hbm, res_ref), (mixg_hbm, mixg_ref), (preg_hbm, preg_ref),
                (postg_hbm, postg_ref), (perm_hbm, perm_ref), (permt_hbm, permt_ref),
            )
        )
    ]
    for load in inputs:
        load.start()

    def weights(i, src, dst):
        return pltpu.make_async_copy(src, dst, wsem.at[i])

    loads = [weights(0, wo_hbm, wo), weights(1, sg_hbm, wg), weights(2, su_hbm, wu), weights(3, sd_hbm, wd)]
    expert_loads = [weights(4, eg_hbm, wg), weights(5, eu_hbm, wu), weights(6, ed_hbm, wd)]

    for load in inputs[:4]:
        load.wait()
    turn = turn_ref[...]
    for g in range(8):
        at = slice(16 * g, 16 * (g + 1))
        q, k, v = (ref[at].reshape(256, 128) for ref in (q_ref, k_ref, v_ref))
        both = jnp.concatenate([q[:, :64], k[:, :64], q[:, 64:], k[:, 64:], v], axis=1)
        rows = dot(turn, both).astype(BF16)
        for part in range(3):
            qkv_send[part, :, at, :] = rows[:, part * 128 : (part + 1) * 128].reshape(16, 16, 128)
    pl.semaphore_wait(barrier, 22)
    for part in range(3):
        for i, d in enumerate(SP_ORDER):
            to = peers.sp(d)
            pltpu.make_async_remote_copy(
                qkv_send.at[part, to], qkv_recv.at[part, sp], qs_sem.at[part, i], qr_sem.at[part, i],
                device_id=(to, dp), device_id_type=MESH,
            ).start()
    for d in range(1, 8):
        pl.semaphore_signal(entered, inc=1, device_id=peers.at(d), device_id_type=MESH)
    for load in loads:
        load.start()
    for part in range(3):
        qkv_recv[part, sp] = qkv_send[part, sp]

    for load in inputs[4:]:
        load.wait()
    oz, oy, ox, oc = (order_ref[i : i + 1, :] for i in range(4))
    mz, my, mx, mc = sp // 4, lax.rem(sp, 4), dp // 2, lax.rem(dp, 2)
    expert = ((oz + mz) & 3) * 32 + ((oy + my) & 3) * 8 + ((ox + mx) & 3) * 2 + ((oc + mc) & 1)
    row_i = lax.broadcasted_iota(I32, (128, 128), 0)
    col_i = lax.broadcasted_iota(I32, (128, 128), 1)
    eye = col_i == row_i

    def as_column(row):
        return jnp.sum(jnp.where(eye, row, jnp.zeros_like(row)), axis=1, keepdims=True)

    hots = [as_column(routes_ref[j : j + 1, :].astype(F32)).astype(I32) == expert for j in range(4)]
    members = sum(h.astype(F32) for h in hots).astype(BF16)
    earlier = dot((col_i < row_i).astype(F32).astype(BF16), members)
    place = earlier + 24.0 * col_i.astype(F32)
    rows_j = []
    for j in range(4):
        r0 = jnp.sum(jnp.where(hots[j], place, 0.0), axis=1, keepdims=True)
        r0b[j] = jnp.broadcast_to(r0, (128, 128)).astype(I32)
        rwb[j] = jnp.broadcast_to(as_column(rw_ref[j : j + 1, :]), (128, 128))
        r0_row = jnp.sum(jnp.where(eye, r0, 0.0), axis=0, keepdims=True).astype(I32)
        rows_j.append(jnp.concatenate([r0_row + 6 * q for q in range(4)], axis=1))

    @pl.loop(0, 24)
    def _(c):
        base = pl.multiple_of(c * 128, 128)
        row = lax.broadcasted_iota(I32, (128, 512), 0) + base
        hit = (row == rows_j[0]) | (row == rows_j[1]) | (row == rows_j[2]) | (row == rows_j[3])
        pick[pl.ds(base, 128), :] = jnp.where(hit, 1.0, 0.0).astype(BF16)

    coef = 0.125 * 1.4426950408889634
    causal = lax.broadcasted_iota(I32, (256, 256), 1) <= lax.broadcasted_iota(I32, (256, 256), 0)

    def exponents(part, t):
        qk = qkv_recv[part, 2 * t : 2 * t + 2].reshape(256, 128)
        q = jnp.concatenate([jnp.zeros((256, 64), BF16), qk[:, :64]], axis=1)
        keys = qkv_recv[part, 0 : 2 * t + 2].reshape(256 * (t + 1), 128)
        s = lax.dot_general(q, keys, (((1,), (1,)), ((), ())), preferred_element_type=F32)
        diag = jnp.where(causal, s[:, t * 256 :], -1e30)
        s = diag if t == 0 else jnp.concatenate([s[:, : t * 256], diag], axis=1)
        p = jnp.exp2((s - jnp.max(s, axis=1, keepdims=True)) * coef)
        return p, jnp.sum(p, axis=1, keepdims=True)

    def tri(t):
        return t * (t + 1) // 2

    for i in range(15):
        landed(qkv_recv.at[0, 0], qr_sem.at[0, i])
    for t in range(8):
        p, l = exponents(0, t)
        l1[t] = jnp.broadcast_to(1.0 / l, (256, 128))
        for c in range(t + 1):
            p1[tri(t) + c] = p[:, c * 256 : (c + 1) * 256]
    for i in range(15):
        landed(qkv_recv.at[1, 0], qr_sem.at[1, i])
    lam = lam_ref[0]
    for t in range(8):
        p, l = exponents(1, t)
        scale1 = jnp.concatenate([l1[t], l1[t]], axis=1)
        scale2 = lam / l
        for c in range(t + 1):
            mixture[tri(t) + c] = (p1[tri(t) + c] * scale1 - p[:, c * 256 : (c + 1) * 256] * scale2).astype(BF16)
    for i in range(15):
        landed(qkv_recv.at[2, 0], qr_sem.at[2, i])
    for t in range(8):
        m = jnp.concatenate([mixture[tri(t) + c] for c in range(t + 1)], axis=1)
        o = dot(m, qkv_recv[2, 0 : 2 * t + 2].reshape(256 * (t + 1), 128))
        head_send[2 * t : 2 * t + 2] = rms(o, hgain_ref[...]).astype(BF16).reshape(2, 128, 128)
    for i, d in enumerate(SP_ORDER):
        to = peers.sp(d)
        pltpu.make_async_remote_copy(
            head_send.at[to], head_recv.at[sp], hs_sem.at[i + 1], hr_sem.at[i + 1],
            device_id=(to, dp), device_id_type=MESH,
        ).start()
    head_recv[sp] = head_send[sp]

    loads[0].wait()
    sources = [sp] + [peers.sp(d, -1) for d in SP_ORDER]
    for i in range(0, 16, 2):
        for n in (i, i + 1):
            if n:
                landed(head_recv.at[0], hr_sem.at[n])
        h0, h1 = sources[i], sources[i + 1]
        x = jnp.concatenate([head_recv[h0], head_recv[h1]], axis=1)
        for c in range(4):
            cols = pl.ds(c * 512, 512)
            part = dot(x, jnp.concatenate([wo[h0, :, cols], wo[h1, :, cols]], axis=0))
            if i == 0:
                acc[:, cols] = part
            else:
                acc[:, cols] += part

    updated = (res_ref[...].astype(F32) + rms(acc[...], mixg_ref[...])).astype(BF16)
    res_ref[...] = updated
    normed = rms(updated.astype(F32), preg_ref[...]).astype(BF16)
    for q in range(4):
        x4[q * 128 : (q + 1) * 128, :] = normed[:, q * 512 : (q + 1) * 512]

    pl.semaphore_wait(entered, 7)
    for g in range(8):
        rows = dot(pick[g * 384 : (g + 1) * 384, :], x4[...]).astype(BF16)
        slab_send[g * 16 : (g + 1) * 16] = rows.reshape(16, 24, 512)
        for at in range(max(1, 16 * g), 16 * g + 16):
            pltpu.make_async_remote_copy(
                slab_send.at[at], slab_recv.at[at], ds_sem.at[0], dr_sem.at[at // 32],
                device_id=peers.at(ALL_ORDER[at]), device_id_type=MESH,
            ).start()
    slab_recv[0] = slab_send[0]

    def hidden_of(x):
        gate, up = dot(x, wg[...]), dot(x, wu[...])
        return (gate / (1.0 + jnp.exp(-gate)) * up).astype(BF16)

    for load in loads[1:]:
        load.wait()
    shared_h = hidden_of(jnp.concatenate([x4[q * 128 : (q + 1) * 128, :] for q in range(4)], axis=1))
    shared[...] = dot(shared_h, wd[...]).astype(BF16)
    for load in expert_loads:
        load.start()

    @pl.loop(0, 12)
    def _(c):
        for half in range(2):
            col = lax.broadcasted_iota(I32, (128, 128), 1) + (c * 256 + half * 128)
            for q in range(4):
                w = jnp.zeros((128, 128), F32)
                for j in range(4):
                    w = jnp.where(col == r0b[j] + 6 * q, rwb[j], w)
                p1[(q // 2) * 12 + c, pl.ds((q % 2) * 128, 128), pl.ds(half * 128, 128)] = w

    for load in expert_loads:
        load.wait()
    for i in range(15):
        for part in range(3):
            landed(qkv_send.at[part, 0], qs_sem.at[part, i])
        landed(head_send.at[0], hs_sem.at[i + 1])

    @pl.loop(0, 4)
    def _(g):
        for gs in range(4):

            @pl.when(g == gs)
            def _():
                lo = max(1, 32 * gs)
                landed(slab_recv.at[pl.ds(lo, 32 * gs + 32 - lo)], dr_sem.at[gs])

        for b in range(4):
            block = slab_recv[pl.ds(g * 32 + b * 8, 8)].reshape(192, 512)
            y = dot(perm_ref[...], block).astype(BF16)
            for q in range(4):
                xs[b * 48 : (b + 1) * 48, q * 512 : (q + 1) * 512] = y[q * 48 : (q + 1) * 48]
        h = hidden_of(xs[...])
        xs[...] = dot(h, wd[...]).astype(BF16)
        for b in range(4):
            y = jnp.concatenate(
                [xs[b * 48 : (b + 1) * 48, q * 512 : (q + 1) * 512] for q in range(4)], axis=0
            )
            back = dot(permt_ref[...], y).astype(BF16)
            slab_recv[pl.ds(g * 32 + b * 8, 8)] = back.reshape(8, 24, 512)
        for gs in range(4):

            @pl.when(g == gs)
            def _():
                for at in range(max(1, 32 * gs), 32 * gs + 32):
                    pltpu.make_async_remote_copy(
                        slab_recv.at[at], res_recv.at[at], rs_sem.at[0], rr_sem.at[at // 16],
                        device_id=peers.at(ALL_ORDER[at], -1), device_id_type=MESH,
                    ).start()

    res_recv[0] = slab_recv[0]

    for u in range(8):
        lo = max(1, 16 * u)
        landed(res_recv.at[pl.ds(lo, 16 * u + 16 - lo)], rr_sem.at[u])
        rows = res_recv[u * 16 : (u + 1) * 16].reshape(384, 512)
        for qq in range(2):
            blocks = [divmod(3 * u + c, 2) for c in range(3)]
            w = jnp.concatenate(
                [p1[qq * 12 + b, :, half * 128 : (half + 1) * 128] for b, half in blocks], axis=1
            )
            hi = w.astype(BF16)
            part = dot(hi, rows) + dot((w - hi.astype(F32)).astype(BF16), rows)
            for q in range(2):
                at = pl.ds((2 * qq + q) * 512, 512)
                if u == 0:
                    acc[:, at] = part[q * 128 : (q + 1) * 128]
                else:
                    acc[:, at] += part[q * 128 : (q + 1) * 128]
    combined = acc[...] + shared[...].astype(F32)
    out_ref[...] = (res_ref[...].astype(F32) + rms(combined, postg_ref[...])).astype(BF16)

    landed(slab_send.at[pl.ds(1, 127)], ds_sem.at[0])
    landed(slab_recv.at[pl.ds(1, 127)], rs_sem.at[0])


def local(
    queries, key_vectors, value_vectors, head_lambda, head_gain, residual, out_weight, mix_gain, pre_gain,
    post_gain, routes, route_weights, expert_gate, expert_up, expert_down, shared_gate, shared_up, shared_down,
):
    order = np.zeros((8, 128), np.int32)
    order[:4] = np.array([digits(k) for k in ALL_ORDER]).T
    perm = np.zeros((192, 192), np.float32)
    for src in range(8):
        for q in range(4):
            for s in range(6):
                perm[q * 48 + src * 6 + s, src * 24 + q * 6 + s] = 1
    turn = np.zeros((256, 256), np.float32)
    for h in range(16):
        for t in range(16):
            turn[h * 16 + t, t * 16 + h] = 1
    vm, hbm = pl.BlockSpec(memory_space=pltpu.VMEM), pl.BlockSpec(memory_space=pl.ANY)
    dma = pltpu.SemaphoreType.DMA
    slabs = pltpu.VMEM((128, 24, 512), BF16)
    heads, wide = pltpu.VMEM((128, 16, 128), BF16), pltpu.VMEM((1, 2048), F32)
    out = pl.pallas_call(
        layer_kernel,
        out_shape=jax.ShapeDtypeStruct((128, 2048), BF16),
        in_specs=[pl.BlockSpec(memory_space=pltpu.SMEM)] + [hbm] * 21,
        out_specs=vm,
        scratch_shapes=[
            heads, heads, heads, pltpu.VMEM((1, 128), F32), pltpu.VMEM((128, 2048), BF16),
            wide, wide, wide, pltpu.VMEM((4, 128), I32), pltpu.VMEM((4, 128), F32), pltpu.VMEM((8, 128), I32),
            pltpu.VMEM((192, 192), BF16), pltpu.VMEM((192, 192), BF16), pltpu.VMEM((256, 256), BF16),
            pltpu.VMEM((16, 128, 2048), BF16),
            pltpu.VMEM((2048, 512), BF16), pltpu.VMEM((2048, 512), BF16), pltpu.VMEM((512, 2048), BF16),
            pltpu.VMEM((3, 16, 128, 128), BF16), pltpu.VMEM((3, 16, 128, 128), BF16),
            pltpu.VMEM((36, 256, 256), F32), pltpu.VMEM((8, 256, 128), F32), pltpu.VMEM((36, 256, 256), BF16),
            pltpu.VMEM((16, 128, 128), BF16), pltpu.VMEM((16, 128, 128), BF16),
            pltpu.VMEM((128, 2048), F32),
            pltpu.VMEM((512, 512), BF16), pltpu.VMEM((3072, 512), BF16),
            slabs, slabs, slabs,
            pltpu.VMEM((192, 2048), BF16), pltpu.VMEM((128, 2048), BF16),
            pltpu.VMEM((4, 128, 128), I32), pltpu.VMEM((4, 128, 128), F32),
            dma((7,)), dma((14,)), dma((3, 15)), dma((3, 15)), dma((16,)), dma((16,)), dma((1,)), dma((4,)), dma((1,)), dma((8,)),
            pltpu.SemaphoreType.REGULAR,
        ],
        compiler_params=pltpu.CompilerParams(
            collective_id=0, has_side_effects=True, vmem_limit_bytes=67043328
        ),
    )(
        head_lambda, queries[0], key_vectors[0], value_vectors[0], head_gain.reshape(1, 128), residual[0],
        mix_gain.reshape(1, -1), pre_gain.reshape(1, -1), post_gain.reshape(1, -1), routes[0].T, route_weights[0].T,
        jnp.asarray(order), jnp.asarray(perm, BF16), jnp.asarray(perm.T, BF16), jnp.asarray(turn, BF16),
        out_weight.reshape(16, 128, 2048), expert_gate[0], expert_up[0], expert_down[0],
        shared_gate, shared_up, shared_down,
    )
    return out.reshape(1, 128, 2048)


def solution(mesh):
    tokens, heads, experts = P("dp", "sp", None), P("dp", "sp", None, None), P(("sp", "dp"), None, None)
    return jax.shard_map(
        local,
        mesh=mesh,
        in_specs=(
            heads, heads, heads, P("sp"), P(), tokens, P(), P(), P(), P(), tokens, tokens,
            experts, experts, experts, P(), P(), P(),
        ),
        out_specs=tokens,
        check_vma=False,
    )
```
